32 devices in a mesh: sp: 8 (over z, x), tp: 4 (over y, core).
Axes of the slice: x: 2, y: 2, z: 4, core: 2. Of those that a mesh axis runs over, the one named last changes fastest.
Arguments:
- queries: bfloat16 [1024, 2048], P('sp', 'tp'), may hold values from -6 to 6
- keys: bfloat16 [1024, 512], P('sp', 'tp'), may hold values from -6 to 6
- values: bfloat16 [1024, 512], P('sp', 'tp'), may hold values from -6 to 6
- break_bias: float32 [16], P('tp'), as said below
- residual: bfloat16 [1024, 4096], P(('sp', 'tp')), may hold values from -6 to 6
- w_out: bfloat16 [2048, 4096], P('tp'), may hold values from -0.125 to 0.125
- ffn_gain: float32 [4096], replicated, may hold values from 0.1 to 1.9
- pick_ids: int32 [1024, 2], P('sp'), may hold values from 0 to 7, as said below
- pair_logit: float32 [1024], P('sp'), may hold values from -8 to 8
- w_gate: bfloat16 [8, 4096, 1024], P('sp', None, 'tp'), may hold values from -0.09375 to 0.09375
- w_up: bfloat16 [8, 4096, 1024], P('sp', None, 'tp'), may hold values from -0.09375 to 0.09375
- w_down: bfloat16 [8, 1024, 4096], P('sp', 'tp'), may hold values from -0.1875 to 0.1875
- out_gain: float32 [4096], replicated, may hold values from 0.1 to 1.9
Outputs:
- new_stream: bfloat16 [1024, 4096], P(('sp', 'tp'))
The draws below stay inside these ranges and needn't reach their ends.
Inputs may be any that keep to these rules, and one draw needn't show every extreme that they name: `break_bias`: the logarithm of a break rate per position: between ln(0.02 / 1024) and ln(8 / 128). `pick_ids`: A row's 2 experts differ and lie in one group of 2 consecutive experts. In each aligned block of 32 rows no expert is named more than 12 times, and some expert exactly 12 times.
All inputs are finite; a program needn't handle non-finite values.
Results may differ from the reference program's by a relative error of at most 0.017.
Values may be sent and summed in bfloat16 or wider, within the bound.
A program may use at most 64 MiB of HBM per device.

```python
import jax
import jax.numpy as jnp
from jax import lax

D = 4096
HEAD = 128
HEADS = 16
KV_HEADS = 4
FF = 1024
GROUPS = 4
TOP = 2
TOK_DEV = 128
TOKENS = 1024
EXPERTS = 8
PER = 2
ROWS_DEV = 32
CAP = 12
N_SP = 8
N_TP = 4


def draw_break_bias(key, part):
    key_kind, key_fast, key_slow = jax.random.split(key, 3)
    fast_share = 0.5
    fast = jax.random.uniform(key_kind, (HEADS,), jnp.float32) < fast_share
    fast_rate = jax.random.uniform(key_fast, (HEADS,), jnp.float32, 3.0, 8.0) / TOK_DEV
    slow_rate = jax.random.uniform(key_slow, (HEADS,), jnp.float32, 0.02, 0.2) / TOKENS
    return jnp.log(jnp.where(fast, fast_rate, slow_rate)).astype(jnp.float32)


def pick_block(key):
    pairs = EXPERTS * CAP // 2
    half_group = PER // 2
    key_label, key_force, key_rank, key_rows = jax.random.split(key, 4)
    rounds = GROUPS * CAP
    labels = jax.vmap(lambda sub_key: jax.random.permutation(sub_key, PER))(jax.random.split(key_label, rounds))
    index = jnp.arange(pairs, dtype=jnp.int32)
    round_id = index // half_group
    inside = index % half_group
    group_id = round_id // CAP
    leading = group_id * PER + labels[round_id, 2 * inside]
    trailing = group_id * PER + labels[round_id, 2 * inside + 1]
    forced = jax.random.randint(key_force, (), 0, EXPERTS)
    hit = ((leading == forced) | (trailing == forced)).astype(jnp.int32)
    ranks = jax.random.permutation(key_rank, pairs).astype(jnp.int32)
    chosen = jnp.argsort(ranks - pairs * hit, stable=True)[:ROWS_DEV]
    chosen = chosen[jax.random.permutation(key_rows, ROWS_DEV)]
    return jnp.stack([leading[chosen], trailing[chosen]], axis=1).astype(jnp.int32)


def draw_pick_ids(key, part):
    blocks = TOKENS // ROWS_DEV
    return jax.vmap(pick_block)(jax.random.split(key, blocks)).reshape(TOKENS, TOP).astype(jnp.int32)


def block_levels(key, shape, cuts, least, largest):
    loudness, own = 1.0, jax.random.fold_in(key, 6)
    for axis_at, blocks in cuts:
        heights = jnp.exp(jax.random.uniform(jax.random.fold_in(own, axis_at), (blocks,), jnp.float32, least / len(cuts), largest / len(cuts)))
        loudness = loudness * jnp.repeat(heights, shape[axis_at] // blocks).reshape([-1 if axis == axis_at else 1 for axis in range(len(shape))])
    return loudness


def centred(rng, dims, scale, most, cuts=(), kind=jnp.bfloat16):
    factor_of = block_levels(rng, dims, cuts, -0.22, 0.18) if cuts else 1.0
    drawn = jax.random.normal(rng, dims, jnp.float32) * scale * factor_of
    return jnp.minimum(jnp.maximum(drawn, -most), most).astype(kind)


def setup_inputs(seed: int = 0) -> dict:
    key_list = jax.random.split(jax.random.key(seed), 14)
    queries = centred(key_list[0], (TOKENS, HEADS * HEAD), 1.0, 6.0, ((0, 8), (1, 4)))
    keys = centred(key_list[1], (TOKENS, KV_HEADS * HEAD), 1.0, 6.0, ((0, 8), (1, 4)))
    values = centred(key_list[2], (TOKENS, KV_HEADS * HEAD), 1.0, 6.0, ((0, 8), (1, 4)))
    break_bias = draw_break_bias(jax.random.fold_in(key_list[13], 71), 0)
    residual = centred(key_list[4], (TOKENS, D), 1.0, 6.0, ((0, 32),))
    w_out = centred(key_list[5], (HEADS * HEAD, D), (HEADS * HEAD) ** -0.5, 0.125, ((0, 4),))
    ffn_gain = jnp.clip(1.0 + 0.18 * jax.random.normal(key_list[6], (D,), jnp.float32), 0.1, 1.9)
    pick_ids = draw_pick_ids(jax.random.fold_in(key_list[13], 71), 0)
    pair_logit = centred(key_list[8], (TOKENS,), 1.5, 8.0, ((0, 8),), jnp.float32)
    w_gate = centred(key_list[9], (EXPERTS, D, FF), D ** -0.5, 0.09375, ((0, 8), (2, 4)))
    w_up = centred(key_list[10], (EXPERTS, D, FF), D ** -0.5, 0.09375, ((0, 8), (2, 4)))
    w_down = centred(key_list[11], (EXPERTS, FF, D), FF ** -0.5, 0.1875, ((0, 8), (1, 4)))
    out_gain = jnp.clip(1.0 + 0.18 * jax.random.normal(key_list[12], (D,), jnp.float32), 0.1, 1.9)
    return {"queries": queries, "keys": keys, "values": values, "break_bias": break_bias, "residual": residual, "w_out": w_out, "ffn_gain": ffn_gain, "pick_ids": pick_ids, "pair_logit": pair_logit, "w_gate": w_gate, "w_up": w_up, "w_down": w_down, "out_gain": out_gain}


epsilon = 1e-06

def rounded(values_in):
    return lax.optimization_barrier(values_in.astype(jnp.bfloat16)).astype(jnp.float32)

def stick_block(carried, query_rows, key_block, value_block, head_bias, query_pos, key_pos):
    output, used_up = carried
    scores = jnp.einsum('qcgd,scd->qcgs', query_rows.astype(jnp.float32), key_block.astype(jnp.float32))
    scores = scores * query_rows.shape[-1] ** (-0.5) + head_bias[None, :, :, None]
    before = (key_pos[None, :] < query_pos[:, None])[:, None, None, :]
    breaks = jnp.where(before, jax.nn.softplus(scores), 0.0)
    behind = lax.cumsum(breaks, axis=3, reverse=True) - breaks
    weights = jnp.where(before, jnp.exp(jax.nn.log_sigmoid(scores) - behind - used_up[..., None]), 0.0)
    output = output + jnp.einsum('qcgs,scd->qcgd', rounded(weights), value_block.astype(jnp.float32))
    return (output, used_up + lax.optimization_barrier(jnp.sum(breaks, axis=3)))

def reference(queries, keys, values, break_bias, residual, w_out, ffn_gain, pick_ids, pair_logit, w_gate, w_up, w_down, out_gain):
    extent = queries.shape[0]
    per_key = HEADS // KV_HEADS
    window = min(512, extent)
    blocks = extent // window
    query_all = queries.reshape(blocks, window, KV_HEADS, per_key, HEAD)
    key_all = keys.reshape(extent, KV_HEADS, HEAD)
    value_all = values.reshape(extent, KV_HEADS, HEAD)
    head_bias = break_bias.reshape(KV_HEADS, per_key)

    def one_block(block_index):
        query_rows = lax.dynamic_index_in_dim(query_all, block_index, 0, keepdims=False)
        query_pos = block_index * window + jnp.arange(window, dtype=jnp.int32)
        initial = (jnp.zeros((window, KV_HEADS, per_key, HEAD), jnp.float32), jnp.zeros((window, KV_HEADS, per_key), jnp.float32))

        def visit(step_index, carried):
            first_key = ((block_index - step_index) * window).astype(jnp.int32)
            key_block = lax.dynamic_slice_in_dim(key_all, first_key, window, 0)
            value_block = lax.dynamic_slice_in_dim(value_all, first_key, window, 0)
            key_pos = first_key + jnp.arange(window, dtype=jnp.int32)
            return stick_block(carried, query_rows, key_block, value_block, head_bias, query_pos, key_pos)
        return lax.fori_loop(jnp.int32(0), block_index + 1, visit, initial)[0]
    attended = lax.map(one_block, jnp.arange(blocks, dtype=jnp.int32)).reshape(extent, HEADS, HEAD)
    scaled = attended * lax.rsqrt(lax.optimization_barrier(jnp.mean(attended * attended, axis=-1, keepdims=True)) + epsilon)
    head_out = scaled.astype(jnp.bfloat16).reshape(extent, HEADS * HEAD)
    set_width = HEADS * HEAD // N_TP
    mixed = jnp.zeros((extent, D), jnp.float32)
    for member in range(N_TP):
        col_start = member * set_width
        mixed = mixed + rounded(jnp.dot(head_out[:, col_start:col_start + set_width], w_out[col_start:col_start + set_width], preferred_element_type=jnp.float32))
    stream = (residual.astype(jnp.float32) + mixed).astype(jnp.bfloat16)
    stream_float = stream.astype(jnp.float32)
    ffn_in = (stream_float * lax.rsqrt(lax.optimization_barrier(jnp.mean(stream_float * stream_float, axis=-1, keepdims=True)) + epsilon) * ffn_gain).astype(jnp.bfloat16)
    picks_flat = pick_ids.reshape(-1).astype(jnp.int32)
    total_picks = picks_flat.shape[0]
    ordering = jnp.argsort(picks_flat, stable=True).astype(jnp.int32)
    sorted_ids = picks_flat[ordering]
    tallies = lax.optimization_barrier(jnp.sum((picks_flat[None, :] == jnp.arange(EXPERTS, dtype=jnp.int32)[:, None]).astype(jnp.int32), axis=1)).astype(jnp.int32)
    offsets = (jnp.cumsum(tallies) - tallies).astype(jnp.int32)
    within = (jnp.arange(total_picks, dtype=jnp.int32) - offsets[sorted_ids]).astype(jnp.int32)
    room = N_SP * N_TP * CAP
    table = jnp.full((EXPERTS, room), total_picks, jnp.int32).at[sorted_ids, within].set(ordering)
    padded = jnp.concatenate([ffn_in, jnp.zeros((1, D), jnp.bfloat16)], axis=0)
    unit_width = FF // N_TP

    def run_expert(operands):
        row_ids, gate_matrix, up_matrix, down_matrix = operands
        inputs = padded[row_ids // TOP]
        hidden = (jax.nn.silu(jnp.dot(inputs, gate_matrix, preferred_element_type=jnp.float32)) * jnp.dot(inputs, up_matrix, preferred_element_type=jnp.float32)).astype(jnp.bfloat16)
        summed = jnp.zeros((room, D), jnp.float32)
        for member in range(N_TP):
            unit_start = member * unit_width
            summed = summed + rounded(jnp.dot(hidden[:, unit_start:unit_start + unit_width], down_matrix[unit_start:unit_start + unit_width], preferred_element_type=jnp.float32))
        return summed.astype(jnp.bfloat16)
    results = lax.map(run_expert, (table, w_gate, w_up, w_down))
    per_pick = jnp.zeros((total_picks + 1, D), jnp.bfloat16).at[table.reshape(-1)].set(results.reshape(-1, D))
    per_pick = per_pick[:total_picks].astype(jnp.float32).reshape(extent, TOP, D)
    blended = jax.nn.sigmoid(pair_logit)[:, None] * per_pick[:, 0] + jax.nn.sigmoid(-pair_logit)[:, None] * per_pick[:, 1]
    blend_scale = lax.rsqrt(lax.optimization_barrier(jnp.mean(blended * blended, axis=-1, keepdims=True)) + epsilon)
    return (stream_float + blended * blend_scale * out_gain).astype(jnp.bfloat16)
```

```python
import functools

import jax
import jax.numpy as jnp
from jax import lax
from jax.experimental import pallas as pl
from jax.experimental.pallas import tpu as pltpu
from jax.sharding import PartitionSpec as P

HEAD = 128
TOP = 2
MESH = pl.DeviceIdType.MESH
TILES = 4

epsilon = 1e-06


def attend_block(query, key_block, value_block, bias, acc, used, diagonal):
    rows = query.shape[0]
    length = key_block.shape[0]
    scores = lax.dot_general(
        query, key_block, (((1,), (1,)), ((), ())), preferred_element_type=jnp.float32
    )
    scores = scores * HEAD ** (-0.5) + bias
    breaks = jnp.maximum(scores, 0.0) + jnp.log1p(jnp.exp(-jnp.abs(scores)))
    stays = scores - breaks
    if diagonal:
        at_row = lax.broadcasted_iota(jnp.int32, (rows, length), 0) % length
        at_col = lax.broadcasted_iota(jnp.int32, (rows, length), 1)
        before = at_col < at_row
        breaks = jnp.where(before, breaks, 0.0)
    later = (
        lax.broadcasted_iota(jnp.int32, (length, length), 0)
        > lax.broadcasted_iota(jnp.int32, (length, length), 1)
    ).astype(jnp.bfloat16)
    coarse = breaks.astype(jnp.bfloat16)
    fine = (breaks - coarse.astype(jnp.float32)).astype(jnp.bfloat16)
    behind = jnp.dot(coarse, later, preferred_element_type=jnp.float32) + jnp.dot(
        fine, later, preferred_element_type=jnp.float32
    )
    weights = jnp.exp(stays - behind - used[...])
    if diagonal:
        weights = jnp.where(before, weights, 0.0)
    acc[...] += jnp.dot(
        weights.astype(jnp.bfloat16), value_block, preferred_element_type=jnp.float32
    )
    used[...] += behind[:, :1] + breaks[:, :1]


def attention_part(
    n_sp, n_tp, q_ref, k_ref, v_ref, bias_ref, w_ref, res_ref, gain_ref,
    stream_ref, ffn_ref, kv_buf, w_buf, accs, useds, parts, recvs,
    w_sem, kv_send, kv_relay, kv_recv, rs_send, rs_recv,
):
    me, mine = lax.axis_index("sp"), lax.axis_index("tp")
    length = q_ref.shape[0]
    kv_local = k_ref.shape[1] // HEAD
    per_key = q_ref.shape[1] // k_ref.shape[1]
    rows = length // n_tp
    width = w_buf.shape[1]
    cols = width // TILES
    load = pltpu.make_async_copy(w_ref, w_buf, w_sem)
    load.start()
    pair, side = me // 2, me % 2
    mate = me + 1 - 2 * side
    sources = (k_ref, v_ref)

    def direct(kind, target):
        return pltpu.make_async_remote_copy(
            src_ref=sources[kind], dst_ref=kv_buf.at[kind, me],
            send_sem=kv_send.at[kind, target], recv_sem=kv_recv.at[kind, me],
            device_id=(target, mine), device_id_type=MESH,
        )

    def relay(kind, source):
        return pltpu.make_async_remote_copy(
            src_ref=kv_buf.at[kind, source], dst_ref=kv_buf.at[kind, source],
            send_sem=kv_relay.at[kind, source], recv_sem=kv_recv.at[kind, source],
            device_id=(mate, mine), device_id_type=MESH,
        )

    for kind in range(2):
        direct(kind, mate).start()

    def send_on(other, carry):
        for kind in range(2):
            direct(kind, 2 * other + side).start()
        return carry

    lax.fori_loop(pair + 1, n_sp // 2, send_on, 0)

    queries, biases = [], []
    for c in range(kv_local):
        heads = [c * per_key + g for g in range(per_key)]
        queries.append(
            jnp.concatenate([q_ref[:, h * HEAD : (h + 1) * HEAD] for h in heads], axis=0)
        )
        biases.append(
            jnp.concatenate([jnp.full((length, 1), bias_ref[h], jnp.float32) for h in heads], axis=0)
        )
    accs[...] = jnp.zeros_like(accs)
    useds[...] = jnp.zeros_like(useds)
    for c in range(kv_local):
        at = slice(c * HEAD, (c + 1) * HEAD)
        attend_block(
            queries[c], k_ref[:, at], v_ref[:, at], biases[c], accs.at[c], useds.at[c], True
        )

    def visit(step, carry):
        source = me - step
        for kind in range(2):
            relay(kind, source).wait_recv()

        @pl.when(step % 2 == 0)
        def _():
            for kind in range(2):
                relay(kind, source).start()

        for c in range(kv_local):
            at = slice(c * HEAD, (c + 1) * HEAD)
            attend_block(
                queries[c], kv_buf[0, source][:, at], kv_buf[1, source][:, at],
                biases[c], accs.at[c], useds.at[c], False,
            )
        return carry

    lax.fori_loop(1, me + 1, visit, 0)

    @pl.when(side == 0)
    def _():
        for kind in range(2):
            relay(kind, mate).wait_recv()

    pieces = []
    for c in range(kv_local):
        out = accs[c]
        out = out * lax.rsqrt(jnp.mean(out * out, axis=-1, keepdims=True) + epsilon)
        out = out.astype(jnp.bfloat16)
        pieces += [out[g * length : (g + 1) * length] for g in range(per_key)]
    head_out = jnp.concatenate(pieces, axis=1)
    load.wait()

    levels = len(recvs)

    def share(level, tile, i):
        bit = (mine >> level) % 2
        at = pl.ds(tile * cols, cols)
        return pltpu.make_async_remote_copy(
            src_ref=parts[level].at[2 * i + 1 - bit, :, at],
            dst_ref=recvs[level].at[i, :, at],
            send_sem=rs_send.at[level, tile, i], recv_sem=rs_recv.at[level, tile, i],
            device_id=(me, mine + (1 - 2 * bit) * (1 << level)), device_id_type=MESH,
        )

    for tile in range(TILES):
        at = slice(tile * cols, (tile + 1) * cols)
        product = jnp.dot(head_out, w_buf[:, at], preferred_element_type=jnp.float32)
        parts[0][:, :, at] = product.astype(jnp.bfloat16).reshape(n_tp, rows, cols)
        for i in range(n_tp // 2):
            share(0, tile, i).start()
    squares = jnp.zeros((rows, 1), jnp.float32)
    for level in range(levels):
        bit = (mine >> level) % 2
        count = n_tp >> (level + 1)
        for tile in range(TILES):
            at = slice(tile * cols, (tile + 1) * cols)
            for i in range(count):
                share(level, tile, i).wait_recv()
                total = parts[level][2 * i + bit, :, at].astype(jnp.float32) + recvs[level][
                    i, :, at
                ].astype(jnp.float32)
                if level + 1 < levels:
                    parts[level + 1][i, :, at] = total.astype(jnp.bfloat16)
                else:
                    total = (total + res_ref[:, at].astype(jnp.float32)).astype(jnp.bfloat16)
                    stream_ref[:, at] = total
                    total = total.astype(jnp.float32)
                    squares += jnp.sum(total * total, axis=1, keepdims=True)
            if level + 1 < levels:
                for i in range(count // 2):
                    share(level + 1, tile, i).start()
    scale = lax.rsqrt(squares / width + epsilon)
    for tile in range(TILES):
        at = slice(tile * cols, (tile + 1) * cols)
        ffn_ref[:, at] = (
            stream_ref[:, at].astype(jnp.float32) * scale * gain_ref[:, at]
        ).astype(jnp.bfloat16)
    for level in range(levels):
        for tile in range(TILES):
            for i in range(n_tp >> (level + 1)):
                share(level, tile, i).wait_send()
    for kind in range(2):
        direct(kind, mate).wait_send()

    def sent_on(other, carry):
        for kind in range(2):
            direct(kind, 2 * other + side).wait_send()
        return carry

    lax.fori_loop(pair + 1, n_sp // 2, sent_on, 0)

    def relayed(other, carry):
        for kind in range(2):
            relay(kind, 2 * other + side).wait_send()
        return carry

    lax.fori_loop(0, pair, relayed, 0)


def attention_scratch(n_sp, n_tp, length, kv_width, q_width, width):
    rows = length // n_tp
    levels = n_tp.bit_length() - 1
    kv_local = kv_width // HEAD
    stacked = q_width // kv_width * length
    bf16 = jnp.bfloat16
    dma = pltpu.SemaphoreType.DMA
    return [
        pltpu.VMEM((2, n_sp, length, kv_width), bf16),
        pltpu.VMEM((q_width, width), bf16),
        pltpu.VMEM((kv_local, stacked, HEAD), jnp.float32),
        pltpu.VMEM((kv_local, stacked, 1), jnp.float32),
        tuple(pltpu.VMEM((n_tp >> level, rows, width), bf16) for level in range(levels)),
        tuple(pltpu.VMEM((n_tp >> (level + 1), rows, width), bf16) for level in range(levels)),
        dma,
        dma((2, n_sp)),
        dma((2, n_sp)),
        dma((2, n_sp)),
        dma((levels, TILES, n_tp // 2)),
        dma((levels, TILES, n_tp // 2)),
    ]


def attend(queries, keys, values, break_bias, w_out, residual, ffn_gain):
    n_sp, n_tp = lax.axis_size("sp"), lax.axis_size("tp")
    vmem = pl.BlockSpec(memory_space=pltpu.VMEM)
    shape = jax.ShapeDtypeStruct(residual.shape, jnp.bfloat16)
    return pl.pallas_call(
        functools.partial(attention_part, n_sp, n_tp),
        out_shape=(shape, shape),
        in_specs=[
            vmem, vmem, vmem, pl.BlockSpec(memory_space=pltpu.SMEM),
            pl.BlockSpec(memory_space=pl.ANY), vmem, vmem,
        ],
        out_specs=(vmem, vmem),
        scratch_shapes=attention_scratch(
            n_sp, n_tp, queries.shape[0], keys.shape[1], queries.shape[1], w_out.shape[1]
        ),
        compiler_params=pltpu.CompilerParams(
            has_side_effects=True, vmem_limit_bytes=48 * 1024 * 1024
        ),
        name="attend",
    )(queries, keys, values, break_bias, w_out, residual, ffn_gain[None])


def on_device(
    queries,
    keys,
    values,
    break_bias,
    residual,
    w_out,
    ffn_gain,
    pick_ids,
    pair_logit,
    w_gate,
    w_up,
    w_down,
    out_gain,
):
    length = queries.shape[0]
    stream, ffn_in = attend(queries, keys, values, break_bias, w_out, residual, ffn_gain)
    stream_float = stream.astype(jnp.float32)
    quarters = lax.axis_size("tp")
    quarter = lax.axis_index("tp")
    slice_rows = length // quarters
    width = w_out.shape[1]
    experts = lax.axis_size("sp")
    capacity = max(2, (3 * slice_rows + experts - 1) // experts)
    routed = lax.dynamic_slice_in_dim(pick_ids, quarter * slice_rows, slice_rows, 0)[None]
    blocks = routed.shape[0]
    entries = ffn_in.reshape(blocks, slice_rows, width)
    flat_ids = routed.reshape(blocks, slice_rows * TOP)
    places = jnp.arange(slice_rows * TOP, dtype=jnp.int32)
    earlier = places[None, :] < places[:, None]
    matches = (flat_ids[:, :, None] == flat_ids[:, None, :]) & earlier[None]
    ranks = jnp.sum(matches.astype(jnp.int32), axis=2)
    targets = (flat_ids * capacity + ranks).reshape(blocks, slice_rows, TOP)
    block_ids = jnp.arange(blocks, dtype=jnp.int32)[:, None]
    outgoing = jnp.zeros((blocks, experts * capacity, width), jnp.bfloat16)
    for pick_index in range(TOP):
        outgoing = outgoing.at[block_ids, targets[:, :, pick_index]].set(entries)
    arrived = lax.all_to_all(outgoing, "sp", split_axis=1, concat_axis=1, tiled=True).reshape(
        -1, width
    )
    piece = lax.all_gather(arrived, "tp", axis=0, tiled=True)
    gated = jax.nn.silu(jnp.dot(piece, w_gate[0], preferred_element_type=jnp.float32))
    hidden = (gated * jnp.dot(piece, w_up[0], preferred_element_type=jnp.float32)).astype(
        jnp.bfloat16
    )
    results = lax.psum_scatter(
        jnp.dot(hidden, w_down[0], preferred_element_type=jnp.float32).astype(jnp.bfloat16),
        "tp",
        scatter_dimension=0,
        tiled=True,
    )
    returned = lax.all_to_all(results, "sp", split_axis=0, concat_axis=0, tiled=True)
    own_targets = targets[0]
    logits = lax.dynamic_slice_in_dim(pair_logit, quarter * slice_rows, slice_rows, 0)
    leading = returned[own_targets[:, 0]].astype(jnp.float32)
    trailing = returned[own_targets[:, 1]].astype(jnp.float32)
    blended = (
        jax.nn.sigmoid(logits)[:, None] * leading + jax.nn.sigmoid(-logits)[:, None] * trailing
    )
    blend_scale = lax.rsqrt(jnp.mean(blended * blended, axis=-1, keepdims=True) + epsilon)
    return (stream_float + blended * blend_scale * out_gain).astype(jnp.bfloat16)


def solution(mesh):
    placed = (
        P("sp", "tp"),
        P("sp", "tp"),
        P("sp", "tp"),
        P("tp"),
        P(("sp", "tp"), None),
        P("tp", None),
        P(),
        P("sp", None),
        P("sp"),
        P("sp", None, "tp"),
        P("sp", None, "tp"),
        P("sp", "tp", None),
        P(),
    )
    return jax.shard_map(
        on_device, mesh=mesh, in_specs=placed, out_specs=P(("sp", "tp"), None), check_vma=False
    )
```

```python
import functools

import jax
import jax.numpy as jnp
from jax import lax
from jax.experimental import pallas as pl
from jax.experimental.pallas import tpu as pltpu
from jax.sharding import PartitionSpec as P

HEAD = 128
TOP = 2
MESH = pl.DeviceIdType.MESH
TILES = 4
GROUPS = 4

epsilon = 1e-06


def attend_block(query, key_block, value_block, bias, acc, used, diagonal):
    rows = query.shape[0]
    length = key_block.shape[0]
    scores = lax.dot_general(
        query, key_block, (((1,), (1,)), ((), ())), preferred_element_type=jnp.float32
    )
    scores = scores * HEAD ** (-0.5) + bias
    breaks = jnp.maximum(scores, 0.0) + jnp.log1p(jnp.exp(-jnp.abs(scores)))
    stays = scores - breaks
    if diagonal:
        at_row = lax.broadcasted_iota(jnp.int32, (rows, length), 0) % length
        at_col = lax.broadcasted_iota(jnp.int32, (rows, length), 1)
        before = at_col < at_row
        breaks = jnp.where(before, breaks, 0.0)
    later = (
        lax.broadcasted_iota(jnp.int32, (length, length), 0)
        > lax.broadcasted_iota(jnp.int32, (length, length), 1)
    ).astype(jnp.bfloat16)
    coarse = breaks.astype(jnp.bfloat16)
    fine = (breaks - coarse.astype(jnp.float32)).astype(jnp.bfloat16)
    behind = jnp.dot(coarse, later, preferred_element_type=jnp.float32) + jnp.dot(
        fine, later, preferred_element_type=jnp.float32
    )
    weights = jnp.exp(stays - behind - used[...])
    if diagonal:
        weights = jnp.where(before, weights, 0.0)
    acc[...] += jnp.dot(
        weights.astype(jnp.bfloat16), value_block, preferred_element_type=jnp.float32
    )
    used[...] += behind[:, :1] + breaks[:, :1]


def attention_part(
    n_sp, n_tp, q_ref, k_ref, v_ref, bias_ref, w_ref, res_ref, gain_ref,
    stream_ref, ffn_ref, kv_buf, w_buf, accs, useds, parts, recvs,
    w_sem, kv_send, kv_relay, kv_recv, rs_send, rs_recv,
):
    me, mine = lax.axis_index("sp"), lax.axis_index("tp")
    length = q_ref.shape[0]
    kv_local = k_ref.shape[1] // HEAD
    per_key = q_ref.shape[1] // k_ref.shape[1]
    rows = length // n_tp
    width = w_buf.shape[1]
    cols = width // TILES
    load = pltpu.make_async_copy(w_ref, w_buf, w_sem)
    load.start()
    pair, side = me // 2, me % 2
    mate = me + 1 - 2 * side
    sources = (k_ref, v_ref)

    def direct(kind, target):
        return pltpu.make_async_remote_copy(
            src_ref=sources[kind], dst_ref=kv_buf.at[kind, me],
            send_sem=kv_send.at[kind, target], recv_sem=kv_recv.at[kind, me],
            device_id=(target, mine), device_id_type=MESH,
        )

    def relay(kind, source):
        return pltpu.make_async_remote_copy(
            src_ref=kv_buf.at[kind, source], dst_ref=kv_buf.at[kind, source],
            send_sem=kv_relay.at[kind, source], recv_sem=kv_recv.at[kind, source],
            device_id=(mate, mine), device_id_type=MESH,
        )

    for kind in range(2):
        direct(kind, mate).start()

    def send_on(other, carry):
        for kind in range(2):
            direct(kind, 2 * other + side).start()
        return carry

    lax.fori_loop(pair + 1, n_sp // 2, send_on, 0)

    queries, biases = [], []
    for c in range(kv_local):
        heads = [c * per_key + g for g in range(per_key)]
        queries.append(
            jnp.concatenate([q_ref[:, h * HEAD : (h + 1) * HEAD] for h in heads], axis=0)
        )
        biases.append(
            jnp.concatenate([jnp.full((length, 1), bias_ref[h], jnp.float32) for h in heads], axis=0)
        )
    accs[...] = jnp.zeros_like(accs)
    useds[...] = jnp.zeros_like(useds)
    for c in range(kv_local):
        at = slice(c * HEAD, (c + 1) * HEAD)
        attend_block(
            queries[c], k_ref[:, at], v_ref[:, at], biases[c], accs.at[c], useds.at[c], True
        )

    def visit(step, carry):
        source = me - step
        for kind in range(2):
            relay(kind, source).wait_recv()

        @pl.when(step % 2 == 0)
        def _():
            for kind in range(2):
                relay(kind, source).start()

        for c in range(kv_local):
            at = slice(c * HEAD, (c + 1) * HEAD)
            attend_block(
                queries[c], kv_buf[0, source][:, at], kv_buf[1, source][:, at],
                biases[c], accs.at[c], useds.at[c], False,
            )
        return carry

    lax.fori_loop(1, me + 1, visit, 0)

    @pl.when(side == 0)
    def _():
        for kind in range(2):
            relay(kind, mate).wait_recv()

    pieces = []
    for c in range(kv_local):
        out = accs[c]
        out = out * lax.rsqrt(jnp.mean(out * out, axis=-1, keepdims=True) + epsilon)
        out = out.astype(jnp.bfloat16)
        pieces += [out[g * length : (g + 1) * length] for g in range(per_key)]
    head_out = jnp.concatenate(pieces, axis=1)
    load.wait()

    levels = len(recvs)

    def share(level, tile, i):
        bit = (mine >> level) % 2
        at = pl.ds(tile * cols, cols)
        return pltpu.make_async_remote_copy(
            src_ref=parts[level].at[2 * i + 1 - bit, :, at],
            dst_ref=recvs[level].at[i, :, at],
            send_sem=rs_send.at[level, tile, i], recv_sem=rs_recv.at[level, tile, i],
            device_id=(me, mine + (1 - 2 * bit) * (1 << level)), device_id_type=MESH,
        )

    for tile in range(TILES):
        at = slice(tile * cols, (tile + 1) * cols)
        product = jnp.dot(head_out, w_buf[:, at], preferred_element_type=jnp.float32)
        parts[0][:, :, at] = product.astype(jnp.bfloat16).reshape(n_tp, rows, cols)
        for i in range(n_tp // 2):
            share(0, tile, i).start()
    squares = jnp.zeros((rows, 1), jnp.float32)
    for level in range(levels):
        bit = (mine >> level) % 2
        count = n_tp >> (level + 1)
        for tile in range(TILES):
            at = slice(tile * cols, (tile + 1) * cols)
            for i in range(count):
                share(level, tile, i).wait_recv()
                total = parts[level][2 * i + bit, :, at].astype(jnp.float32) + recvs[level][
                    i, :, at
                ].astype(jnp.float32)
                if level + 1 < levels:
                    parts[level + 1][i, :, at] = total.astype(jnp.bfloat16)
                else:
                    total = (total + res_ref[:, at].astype(jnp.float32)).astype(jnp.bfloat16)
                    stream_ref[:, at] = total
                    total = total.astype(jnp.float32)
                    squares += jnp.sum(total * total, axis=1, keepdims=True)
            if level + 1 < levels:
                for i in range(count // 2):
                    share(level + 1, tile, i).start()
    scale = lax.rsqrt(squares / width + epsilon)
    for tile in range(TILES):
        at = slice(tile * cols, (tile + 1) * cols)
        ffn_ref[:, at] = (
            stream_ref[:, at].astype(jnp.float32) * scale * gain_ref[:, at]
        ).astype(jnp.bfloat16)
    for level in range(levels):
        for tile in range(TILES):
            for i in range(n_tp >> (level + 1)):
                share(level, tile, i).wait_send()
    for kind in range(2):
        direct(kind, mate).wait_send()

    def sent_on(other, carry):
        for kind in range(2):
            direct(kind, 2 * other + side).wait_send()
        return carry

    lax.fori_loop(pair + 1, n_sp // 2, sent_on, 0)

    def relayed(other, carry):
        for kind in range(2):
            relay(kind, 2 * other + side).wait_send()
        return carry

    lax.fori_loop(0, pair, relayed, 0)


def attention_scratch(n_sp, n_tp, length, kv_width, q_width, width):
    rows = length // n_tp
    levels = n_tp.bit_length() - 1
    kv_local = kv_width // HEAD
    stacked = q_width // kv_width * length
    bf16 = jnp.bfloat16
    dma = pltpu.SemaphoreType.DMA
    return [
        pltpu.VMEM((2, n_sp, length, kv_width), bf16),
        pltpu.VMEM((q_width, width), bf16),
        pltpu.VMEM((kv_local, stacked, HEAD), jnp.float32),
        pltpu.VMEM((kv_local, stacked, 1), jnp.float32),
        tuple(pltpu.VMEM((n_tp >> level, rows, width), bf16) for level in range(levels)),
        tuple(pltpu.VMEM((n_tp >> (level + 1), rows, width), bf16) for level in range(levels)),
        dma,
        dma((2, n_sp)),
        dma((2, n_sp)),
        dma((2, n_sp)),
        dma((levels, TILES, n_tp // 2)),
        dma((levels, TILES, n_tp // 2)),
    ]


def attend(queries, keys, values, break_bias, w_out, residual, ffn_gain):
    n_sp, n_tp = lax.axis_size("sp"), lax.axis_size("tp")
    vmem = pl.BlockSpec(memory_space=pltpu.VMEM)
    shape = jax.ShapeDtypeStruct(residual.shape, jnp.bfloat16)
    return pl.pallas_call(
        functools.partial(attention_part, n_sp, n_tp),
        out_shape=(shape, shape),
        in_specs=[
            vmem, vmem, vmem, pl.BlockSpec(memory_space=pltpu.SMEM),
            pl.BlockSpec(memory_space=pl.ANY), vmem, vmem,
        ],
        out_specs=(vmem, vmem),
        scratch_shapes=attention_scratch(
            n_sp, n_tp, queries.shape[0], keys.shape[1], queries.shape[1], w_out.shape[1]
        ),
        compiler_params=pltpu.CompilerParams(
            has_side_effects=True, vmem_limit_bytes=48 * 1024 * 1024
        ),
        name="attend",
    )(queries, keys, values, break_bias, w_out, residual, ffn_gain[None])


def expert_part(
    capacity, place_ref, back_ref, weight_ref, ffn_ref, stream_ref, gain_ref, gate_ref, up_ref, down_ref,
    out_ref, gate_buf, up_buf, down_buf, own, packed, landed, slabs, outs, first, total,
    corner, direct, giving, leaving, given, staged, blend, load_sem, send_sem, recv_sem,
):
    me, mine = lax.axis_index("sp"), lax.axis_index("tp")
    group, member = me // TOP, me % TOP
    across, core = mine // 2, mine % 2
    groups = packed.shape[0]
    half = blend.shape[2]
    rows = ffn_ref.shape[0]
    wide = packed.shape[2]
    cuts = (slice(0, half // 2), slice(half // 2, wide))
    thin = (slice(0, half // 2), slice(half // 2, half))
    x_side = (me + 1 - 2 * member, mine)
    y_side = (me, mine + 2 - 4 * across)
    twin = (me, mine + 1 - 2 * core)
    sent = []

    def send(src, dst, device):
        copy = pltpu.make_async_remote_copy(
            src_ref=src, dst_ref=dst, send_sem=send_sem.at[len(sent)],
            recv_sem=recv_sem.at[len(sent)], device_id=device, device_id_type=MESH,
        )
        copy.start()
        sent.append(copy)
        return copy

    def columns(side):
        return pl.ds(pl.multiple_of(side * half, half), half)

    swap = send(ffn_ref.at[:, columns(1 - core)], own.at[core], twin)
    loads = []
    for at, (src, dst) in enumerate(((gate_ref, gate_buf), (up_ref, up_buf), (down_ref, down_buf))):
        loads.append(pltpu.make_async_copy(src, dst, load_sem.at[at]))
        loads[-1].start()
    kept = ffn_ref[:, columns(core)]
    place = place_ref[...]
    slots = packed.shape[1]
    tail = jnp.dot(place, weight_ref[...], preferred_element_type=jnp.float32)
    for g in range(groups):
        packed[g, :, half:] = tail[g * slots : (g + 1) * slots].astype(jnp.bfloat16)
    swap.wait_recv()
    other = own[1 - core]
    lead = jnp.where(core == 0, kept, other)
    rest = jnp.where(core == 0, other, kept)
    joined = jnp.concatenate([lead, rest], axis=0)
    moved = []
    for cut, body in zip(cuts, thin):
        rows_out = jnp.dot(place, joined[:, body], preferred_element_type=jnp.float32)
        for g in range(groups):
            packed[g, :, body] = rows_out[g * slots : (g + 1) * slots].astype(jnp.bfloat16)
        step = []
        for hop in range(1, groups):
            target = (group + hop) % groups
            step.append(
                send(packed.at[target, :, cut], landed.at[group, :, cut], (target * TOP + member, mine))
            )
        moved.append(step)
        landed[group, :, cut] = packed[group, :, cut]
    beside_x, beside_y, far, shared = [], [], [], []
    for cut, step in zip(cuts, moved):
        for copy in step:
            copy.wait_recv()
        whole = jnp.concatenate(
            [landed[g, :, cut].astype(jnp.float32) for g in range(groups)], axis=0
        )
        slabs[core, member, across, :, cut] = whole.astype(jnp.bfloat16)
        here = slabs.at[core, member, across, :, cut]
        beside_x.append(send(here, here, x_side))
        beside_y.append(send(here, here, y_side))
        shared.append(send(here, here, twin))
    for at, cut in enumerate(cuts):
        from_y = slabs.at[core, member, 1 - across, :, cut]
        from_x = slabs.at[core, 1 - member, across, :, cut]
        beside_y[at].wait_recv()
        if at == 0:
            far.append(send(from_y, from_y, x_side))
        shared.append(send(from_y, from_y, twin))
        beside_x[at].wait_recv()
        if at == 1:
            far.append(send(from_x, from_x, y_side))
    for at, cut in enumerate(cuts):
        from_x = slabs.at[core, 1 - member, across, :, cut]
        shared.append(send(from_x, from_x, twin))
    for copy in loads:
        copy.wait()

    def run(which):
        lefts = [slabs[side, which].reshape(-1, wide) for side in range(2)]
        gate, up = (
            sum(
                jnp.dot(
                    lefts[side][:, :half], buf[side * half : (side + 1) * half],
                    preferred_element_type=jnp.float32,
                )
                for side in range(2)
            )
            for buf in (gate_buf, up_buf)
        )
        hidden = (gate / (1.0 + jnp.exp(-gate)) * up).astype(jnp.bfloat16)
        shares = lefts[0][:, half : half + HEAD].astype(jnp.float32)
        share = jnp.where(
            member == 0, shares[:, 0:1] + shares[:, 1:2], shares[:, 2:3] + shares[:, 3:4]
        )
        for side in range(2):
            for body in thin:
                at = slice(side * half + body.start, side * half + body.stop)
                result = jnp.dot(hidden, down_buf[:, at], preferred_element_type=jnp.float32)
                result = (result * share).astype(jnp.bfloat16)
                outs[side, which, :, :, body] = result.reshape(2, -1, half // 2)

    for copy in shared[:4]:
        copy.wait_recv()
    run(member)
    for at, cut in enumerate(cuts):
        far[at].wait_recv()
        diagonal = slabs.at[core, 1 - member, 1 - across, :, cut]
        shared.append(send(diagonal, diagonal, twin))
    sums = []
    sums.append([
        send(outs.at[1 - core, member, :, :, body], first.at[member, :, :, body], twin)
        for body in thin
    ])
    for copy in shared[4:]:
        copy.wait_recv()
    run(1 - member)
    sums.append([
        send(outs.at[1 - core, 1 - member, :, :, body], first.at[1 - member, :, :, body], twin)
        for body in thin
    ])
    real = jnp.float32
    for copies, which in zip(sums, (member, 1 - member)):
        for copy, body in zip(copies, thin):
            copy.wait_recv()
            added = outs[core, which, :, :, body].astype(real) + first[which, :, :, body].astype(real)
            total[which, :, :, body] = added.astype(jnp.bfloat16)
    diagonal = total.at[1 - member, 1 - across]
    to_y = send(diagonal.at[:, thin[0]], corner.at[0], y_side)
    to_x = send(diagonal.at[:, thin[1]], corner.at[1], x_side)
    x_slab = total.at[1 - member, across]
    y_slab = total.at[member, 1 - across]
    got = [[None, None], [None, None]]
    got[0][1] = send(x_slab.at[:, thin[1]], direct.at[0, :, thin[1]], x_side)
    got[1][0] = send(y_slab.at[:, thin[0]], direct.at[1, :, thin[0]], y_side)
    to_y.wait_recv()
    giving[0] = (total[1 - member, across, :, thin[0]].astype(real) + corner[0].astype(real)).astype(jnp.bfloat16)
    got[0][0] = send(giving.at[0], direct.at[0, :, thin[0]], x_side)
    to_x.wait_recv()
    giving[1] = (total[member, 1 - across, :, thin[1]].astype(real) + corner[1].astype(real)).astype(jnp.bfloat16)
    got[1][1] = send(giving.at[1], direct.at[1, :, thin[1]], y_side)
    for at, body in enumerate(thin):
        got[0][at].wait_recv()
        got[1][at].wait_recv()
        final = (
            total[member, across, :, body].astype(real)
            + direct[0, :, body].astype(real)
            + direct[1, :, body].astype(real)
        )
        for g in range(groups):
            leaving[g, :, body] = final[g * slots : (g + 1) * slots].astype(jnp.bfloat16)
    returns = []
    for body in thin:
        step = []
        for hop in range(1, groups):
            target = (group + hop) % groups
            step.append(
                send(leaving.at[target, :, body], given.at[group, :, body], (target * TOP + member, mine))
            )
        returns.append(step)
        given[group, :, body] = leaving[group, :, body]
    for body, step in zip(thin, returns):
        for copy in step:
            copy.wait_recv()
        whole = jnp.concatenate([given[g, :, body].astype(real) for g in range(groups)], axis=0)
        back = jnp.dot(back_ref[...], whole.astype(jnp.bfloat16), preferred_element_type=real)
        staged[:, :, body] = back.astype(jnp.bfloat16).reshape(2, rows, half // 2)
    last = send(staged.at[1 - core], blend.at[core], twin)
    squares = jnp.sum(staged[core].astype(real) ** 2, axis=1, keepdims=True)
    last.wait_recv()
    squares += jnp.sum(blend[1 - core].astype(real) ** 2, axis=1, keepdims=True)
    scale = lax.rsqrt(squares / (2 * half) + epsilon)
    for side, source in ((core, staged), (1 - core, blend)):
        at = columns(side)
        out_ref[:, at] = (
            stream_ref[:, at].astype(real) + source[side].astype(real) * scale * gain_ref[:, at]
        ).astype(jnp.bfloat16)
    for copy in sent:
        copy.wait_send()


def grouped_experts(capacity, ffn_in, stream, pick_ids, pair_logit, w_gate, w_up, w_down, out_gain):
    rows, width = stream.shape
    groups = lax.axis_size("sp") // TOP
    across = lax.axis_index("tp") // 2
    chip_rows, slots, half = 2 * rows, 2 * capacity, width // 2
    picks = lax.dynamic_slice_in_dim(pick_ids, across * chip_rows, chip_rows, 0)
    logits = lax.dynamic_slice_in_dim(pair_logit, across * chip_rows, chip_rows, 0)
    chosen = picks[:, 0] // TOP
    at = jnp.arange(chip_rows, dtype=jnp.int32)
    same = (chosen[None, :] == chosen[:, None]) & (at[None, :] < at[:, None])
    target = chosen * slots + jnp.sum(same.astype(jnp.int32), axis=1)
    place = (target[None, :] == jnp.arange(groups * slots, dtype=jnp.int32)[:, None]).astype(jnp.bfloat16)
    sign = jnp.where(picks[:, 0] % TOP == 0, 1.0, -1.0)
    shares = jnp.stack([jax.nn.sigmoid(sign * logits), jax.nn.sigmoid(-sign * logits)], axis=1)
    coarse = lax.reduce_precision(shares, 8, 7)
    parts = jnp.stack([coarse, shares - coarse], axis=2).reshape(chip_rows, 2 * TOP)
    parts = jnp.pad(parts.astype(jnp.bfloat16), ((0, 0), (0, HEAD - 2 * TOP)))
    vmem = pl.BlockSpec(memory_space=pltpu.VMEM)
    hbm = pl.BlockSpec(memory_space=pl.ANY)
    block = groups * slots

    def room(*shape):
        return pltpu.VMEM(shape, jnp.bfloat16)

    dma = pltpu.SemaphoreType.DMA
    return pl.pallas_call(
        functools.partial(expert_part, capacity),
        out_shape=jax.ShapeDtypeStruct(stream.shape, jnp.bfloat16),
        in_specs=[vmem] * 6 + [hbm] * 3,
        out_specs=vmem,
        scratch_shapes=[
            room(*w_gate.shape), room(*w_up.shape), room(*w_down.shape),
            room(2, rows, half),
            room(groups, slots, half + HEAD),
            room(groups, slots, half + HEAD),
            room(2, TOP, 2, block, half + HEAD),
            room(2, TOP, 2, block, half),
            room(TOP, 2, block, half),
            room(TOP, 2, block, half),
            room(2, block, half // 2),
            room(2, block, half),
            room(2, block, half // 2),
            room(groups, slots, half),
            room(groups, slots, half),
            room(2, rows, half),
            room(2, rows, half),
            dma((3,)), dma((64,)), dma((64,)),
        ],
        compiler_params=pltpu.CompilerParams(
            has_side_effects=True, vmem_limit_bytes=56 * 1024 * 1024
        ),
        name="experts",
    )(place, place.T, parts, ffn_in, stream, out_gain[None], w_gate, w_up, w_down)


def on_device(
    queries,
    keys,
    values,
    break_bias,
    residual,
    w_out,
    ffn_gain,
    pick_ids,
    pair_logit,
    w_gate,
    w_up,
    w_down,
    out_gain,
):
    length = queries.shape[0]
    stream, ffn_in = attend(queries, keys, values, break_bias, w_out, residual, ffn_gain)
    stream_float = stream.astype(jnp.float32)
    quarters = lax.axis_size("tp")
    quarter = lax.axis_index("tp")
    slice_rows = length // quarters
    width = w_out.shape[1]
    experts = lax.axis_size("sp")
    capacity = max(2, (3 * slice_rows + experts - 1) // experts)
    if experts == GROUPS * TOP and quarters == 4:
        return grouped_experts(
            capacity, ffn_in, stream, pick_ids, pair_logit, w_gate[0], w_up[0], w_down[0], out_gain
        )
    routed = lax.dynamic_slice_in_dim(pick_ids, quarter * slice_rows, slice_rows, 0)[None]
    blocks = routed.shape[0]
    entries = ffn_in.reshape(blocks, slice_rows, width)
    flat_ids = routed.reshape(blocks, slice_rows * TOP)
    places = jnp.arange(slice_rows * TOP, dtype=jnp.int32)
    earlier = places[None, :] < places[:, None]
    matches = (flat_ids[:, :, None] == flat_ids[:, None, :]) & earlier[None]
    ranks = jnp.sum(matches.astype(jnp.int32), axis=2)
    targets = (flat_ids * capacity + ranks).reshape(blocks, slice_rows, TOP)
    block_ids = jnp.arange(blocks, dtype=jnp.int32)[:, None]
    outgoing = jnp.zeros((blocks, experts * capacity, width), jnp.bfloat16)
    for pick_index in range(TOP):
        outgoing = outgoing.at[block_ids, targets[:, :, pick_index]].set(entries)
    arrived = lax.all_to_all(outgoing, "sp", split_axis=1, concat_axis=1, tiled=True).reshape(
        -1, width
    )
    piece = lax.all_gather(arrived, "tp", axis=0, tiled=True)
    gated = jax.nn.silu(jnp.dot(piece, w_gate[0], preferred_element_type=jnp.float32))
    hidden = (gated * jnp.dot(piece, w_up[0], preferred_element_type=jnp.float32)).astype(
        jnp.bfloat16
    )
    results = lax.psum_scatter(
        jnp.dot(hidden, w_down[0], preferred_element_type=jnp.float32).astype(jnp.bfloat16),
        "tp",
        scatter_dimension=0,
        tiled=True,
    )
    returned = lax.all_to_all(results, "sp", split_axis=0, concat_axis=0, tiled=True)
    own_targets = targets[0]
    logits = lax.dynamic_slice_in_dim(pair_logit, quarter * slice_rows, slice_rows, 0)
    leading = returned[own_targets[:, 0]].astype(jnp.float32)
    trailing = returned[own_targets[:, 1]].astype(jnp.float32)
    blended = (
        jax.nn.sigmoid(logits)[:, None] * leading + jax.nn.sigmoid(-logits)[:, None] * trailing
    )
    blend_scale = lax.rsqrt(jnp.mean(blended * blended, axis=-1, keepdims=True) + epsilon)
    return (stream_float + blended * blend_scale * out_gain).astype(jnp.bfloat16)


def solution(mesh):
    placed = (
        P("sp", "tp"),
        P("sp", "tp"),
        P("sp", "tp"),
        P("tp"),
        P(("sp", "tp"), None),
        P("tp", None),
        P(),
        P("sp", None),
        P("sp"),
        P("sp", None, "tp"),
        P("sp", None, "tp"),
        P("sp", "tp", None),
        P(),
    )
    return jax.shard_map(
        on_device, mesh=mesh, in_specs=placed, out_specs=P(("sp", "tp"), None), check_vma=False
    )
```

```python
import functools

import jax
import jax.numpy as jnp
from jax import lax
from jax.experimental import pallas as pl
from jax.experimental.pallas import tpu as pltpu
from jax.sharding import PartitionSpec as P

HEAD = 128
TOP = 2
MESH = pl.DeviceIdType.MESH
TILES = 4
GROUPS = 4

epsilon = 1e-06


def attend_block(query, key_block, value_block, bias, acc, used, diagonal):
    rows = query.shape[0]
    length = key_block.shape[0]
    scores = lax.dot_general(
        query, key_block, (((1,), (1,)), ((), ())), preferred_element_type=jnp.float32
    )
    scores = scores * HEAD ** (-0.5) + bias
    breaks = jnp.maximum(scores, 0.0) + jnp.log(1.0 + jnp.exp(-jnp.abs(scores)))
    stays = scores - breaks
    if diagonal:
        at_row = lax.broadcasted_iota(jnp.int32, (rows, length), 0) % length
        at_col = lax.broadcasted_iota(jnp.int32, (rows, length), 1)
        before = at_col < at_row
        breaks = jnp.where(before, breaks, 0.0)
    later = (
        lax.broadcasted_iota(jnp.int32, (length, length), 0)
        > lax.broadcasted_iota(jnp.int32, (length, length), 1)
    ).astype(jnp.bfloat16)
    coarse = breaks.astype(jnp.bfloat16)
    fine = (breaks - coarse.astype(jnp.float32)).astype(jnp.bfloat16)
    behind = jnp.dot(coarse, later, preferred_element_type=jnp.float32) + jnp.dot(
        fine, later, preferred_element_type=jnp.float32
    )
    weights = jnp.exp(stays - behind - used[...])
    if diagonal:
        weights = jnp.where(before, weights, 0.0)
    acc[...] += jnp.dot(
        weights.astype(jnp.bfloat16), value_block, preferred_element_type=jnp.float32
    )
    used[...] += behind[:, :1] + breaks[:, :1]


def attention_part(
    n_sp, n_tp, q_hbm, k_hbm, v_hbm, bias_ref, w_ref, res_hbm, gain_hbm,
    stream_ref, ffn_ref, q_ref, k_ref, v_ref, res_ref, gain_ref, in_sem, kv_buf, w_buf, accs, useds, parts, recvs,
    w_sem, kv_send, kv_relay, kv_recv, rs_send, rs_recv,
):
    me, mine = lax.axis_index("sp"), lax.axis_index("tp")
    length = q_ref.shape[0]
    kv_local = k_ref.shape[1] // HEAD
    per_key = q_ref.shape[1] // k_ref.shape[1]
    rows = length // n_tp
    width = w_buf.shape[1]
    cols = width // TILES
    arriving = [
        pltpu.make_async_copy(src, dst, in_sem.at[at])
        for at, (src, dst) in enumerate((
            (k_hbm, k_ref), (v_hbm, v_ref), (q_hbm, q_ref), (res_hbm, res_ref), (gain_hbm, gain_ref),
        ))
    ]
    for copy in arriving:
        copy.start()
    load = pltpu.make_async_copy(w_ref, w_buf, w_sem)
    load.start()
    for copy in arriving[:2]:
        copy.wait()
    pair, side = me // 2, me % 2
    mate = me + 1 - 2 * side
    sources = (k_ref, v_ref)

    def direct(kind, target):
        return pltpu.make_async_remote_copy(
            src_ref=sources[kind], dst_ref=kv_buf.at[kind, me],
            send_sem=kv_send.at[kind, target], recv_sem=kv_recv.at[kind, me],
            device_id=(target, mine), device_id_type=MESH,
        )

    def relay(kind, source):
        return pltpu.make_async_remote_copy(
            src_ref=kv_buf.at[kind, source], dst_ref=kv_buf.at[kind, source],
            send_sem=kv_relay.at[kind, source], recv_sem=kv_recv.at[kind, source],
            device_id=(mate, mine), device_id_type=MESH,
        )

    for kind in range(2):
        direct(kind, mate).start()

    def send_on(other, carry):
        for kind in range(2):
            direct(kind, 2 * other + side).start()
        return carry

    lax.fori_loop(pair + 1, n_sp // 2, send_on, 0)

    arriving[2].wait()
    queries, biases = [], []
    for c in range(kv_local):
        heads = [c * per_key + g for g in range(per_key)]
        queries.append(
            jnp.concatenate([q_ref[:, h * HEAD : (h + 1) * HEAD] for h in heads], axis=0)
        )
        biases.append(
            jnp.concatenate([jnp.full((length, 1), bias_ref[h], jnp.float32) for h in heads], axis=0)
        )
    accs[...] = jnp.zeros_like(accs)
    useds[...] = jnp.zeros_like(useds)
    for c in range(kv_local):
        at = slice(c * HEAD, (c + 1) * HEAD)
        attend_block(
            queries[c], k_ref[:, at], v_ref[:, at], biases[c], accs.at[c], useds.at[c], True
        )

    def visit(step, carry):
        source = me - step
        for kind in range(2):
            relay(kind, source).wait_recv()

        @pl.when(step % 2 == 0)
        def _():
            for kind in range(2):
                relay(kind, source).start()

        for c in range(kv_local):
            at = slice(c * HEAD, (c + 1) * HEAD)
            attend_block(
                queries[c], kv_buf[0, source][:, at], kv_buf[1, source][:, at],
                biases[c], accs.at[c], useds.at[c], False,
            )
        return carry

    lax.fori_loop(1, me + 1, visit, 0)

    @pl.when(side == 0)
    def _():
        for kind in range(2):
            relay(kind, mate).wait_recv()

    pieces = []
    for c in range(kv_local):
        out = accs[c]
        out = out * lax.rsqrt(jnp.mean(out * out, axis=-1, keepdims=True) + epsilon)
        out = out.astype(jnp.bfloat16)
        pieces += [out[g * length : (g + 1) * length] for g in range(per_key)]
    head_out = jnp.concatenate(pieces, axis=1)
    load.wait()

    levels = len(recvs)

    def share(level, tile, i):
        bit = (mine >> level) % 2
        at = pl.ds(tile * cols, cols)
        return pltpu.make_async_remote_copy(
            src_ref=parts[level].at[2 * i + 1 - bit, :, at],
            dst_ref=recvs[level].at[i, :, at],
            send_sem=rs_send.at[level, tile, i], recv_sem=rs_recv.at[level, tile, i],
            device_id=(me, mine + (1 - 2 * bit) * (1 << level)), device_id_type=MESH,
        )

    for tile in range(TILES):
        at = slice(tile * cols, (tile + 1) * cols)
        product = jnp.dot(head_out, w_buf[:, at], preferred_element_type=jnp.float32)
        parts[0][:, :, at] = product.astype(jnp.bfloat16).reshape(n_tp, rows, cols)
        for i in range(n_tp // 2):
            share(0, tile, i).start()
    for copy in arriving[3:]:
        copy.wait()
    squares = jnp.zeros((rows, 1), jnp.float32)
    for level in range(levels):
        bit = (mine >> level) % 2
        count = n_tp >> (level + 1)
        for tile in range(TILES):
            at = slice(tile * cols, (tile + 1) * cols)
            for i in range(count):
                share(level, tile, i).wait_recv()
                total = parts[level][2 * i + bit, :, at].astype(jnp.float32) + recvs[level][
                    i, :, at
                ].astype(jnp.float32)
                if level + 1 < levels:
                    parts[level + 1][i, :, at] = total.astype(jnp.bfloat16)
                else:
                    total = (total + res_ref[:, at].astype(jnp.float32)).astype(jnp.bfloat16)
                    stream_ref[:, at] = total
                    total = total.astype(jnp.float32)
                    squares += jnp.sum(total * total, axis=1, keepdims=True)
            if level + 1 < levels:
                for i in range(count // 2):
                    share(level + 1, tile, i).start()
    scale = lax.rsqrt(squares / width + epsilon)
    for tile in range(TILES):
        at = slice(tile * cols, (tile + 1) * cols)
        ffn_ref[:, at] = (
            stream_ref[:, at].astype(jnp.float32) * scale * gain_ref[:, at]
        ).astype(jnp.bfloat16)
    for level in range(levels):
        for tile in range(TILES):
            for i in range(n_tp >> (level + 1)):
                share(level, tile, i).wait_send()
    for kind in range(2):
        direct(kind, mate).wait_send()

    def sent_on(other, carry):
        for kind in range(2):
            direct(kind, 2 * other + side).wait_send()
        return carry

    lax.fori_loop(pair + 1, n_sp // 2, sent_on, 0)

    def relayed(other, carry):
        for kind in range(2):
            relay(kind, 2 * other + side).wait_send()
        return carry

    lax.fori_loop(0, pair, relayed, 0)


def attention_scratch(n_sp, n_tp, length, kv_width, q_width, width):
    rows = length // n_tp
    levels = n_tp.bit_length() - 1
    kv_local = kv_width // HEAD
    stacked = q_width // kv_width * length
    bf16 = jnp.bfloat16
    dma = pltpu.SemaphoreType.DMA
    return [
        pltpu.VMEM((length, q_width), bf16),
        pltpu.VMEM((length, kv_width), bf16),
        pltpu.VMEM((length, kv_width), bf16),
        pltpu.VMEM((rows, width), bf16),
        pltpu.VMEM((1, width), jnp.float32),
        dma((5,)),
        pltpu.VMEM((2, n_sp, length, kv_width), bf16),
        pltpu.VMEM((q_width, width), bf16),
        pltpu.VMEM((kv_local, stacked, HEAD), jnp.float32),
        pltpu.VMEM((kv_local, stacked, 1), jnp.float32),
        tuple(pltpu.VMEM((n_tp >> level, rows, width), bf16) for level in range(levels)),
        tuple(pltpu.VMEM((n_tp >> (level + 1), rows, width), bf16) for level in range(levels)),
        dma,
        dma((2, n_sp)),
        dma((2, n_sp)),
        dma((2, n_sp)),
        dma((levels, TILES, n_tp // 2)),
        dma((levels, TILES, n_tp // 2)),
    ]


def attend(queries, keys, values, break_bias, w_out, residual, ffn_gain):
    n_sp, n_tp = lax.axis_size("sp"), lax.axis_size("tp")
    vmem = pl.BlockSpec(memory_space=pltpu.VMEM)
    hbm = pl.BlockSpec(memory_space=pl.ANY)
    shape = jax.ShapeDtypeStruct(residual.shape, jnp.bfloat16)
    return pl.pallas_call(
        functools.partial(attention_part, n_sp, n_tp),
        out_shape=(shape, shape),
        in_specs=[hbm, hbm, hbm, pl.BlockSpec(memory_space=pltpu.SMEM), hbm, hbm, hbm],
        out_specs=(vmem, vmem),
        scratch_shapes=attention_scratch(
            n_sp, n_tp, queries.shape[0], keys.shape[1], queries.shape[1], w_out.shape[1]
        ),
        compiler_params=pltpu.CompilerParams(
            has_side_effects=True, vmem_limit_bytes=63 * 1024 * 1024
        ),
        name="attend",
    )(queries, keys, values, break_bias, w_out, residual, ffn_gain[None])


def expert_part(
    place_ref, back_ref, weight_ref, ffn_ref, stream_ref, gain_ref, gate_ref, up_ref, down_ref,
    out_ref, gate_buf, up_buf, down_buf, own, packed, landed, slabs, outs, first, total,
    corner, direct, giving, leaving, given, staged, blend, load_sem, send_sem, recv_sem,
):
    me, mine = lax.axis_index("sp"), lax.axis_index("tp")
    group, member = me // TOP, me % TOP
    across, core = mine // 2, mine % 2
    groups = packed.shape[0]
    half = blend.shape[2]
    rows = ffn_ref.shape[0]
    wide = packed.shape[2]
    cuts = (slice(0, half // 2), slice(half // 2, wide))
    thin = (slice(0, half // 2), slice(half // 2, half))
    x_side = (me + 1 - 2 * member, mine)
    y_side = (me, mine + 2 - 4 * across)
    twin = (me, mine + 1 - 2 * core)
    sent = []

    def send(src, dst, device):
        copy = pltpu.make_async_remote_copy(
            src_ref=src, dst_ref=dst, send_sem=send_sem.at[len(sent)],
            recv_sem=recv_sem.at[len(sent)], device_id=device, device_id_type=MESH,
        )
        copy.start()
        sent.append(copy)
        return copy

    def columns(side):
        return pl.ds(pl.multiple_of(side * half, half), half)

    swap = send(ffn_ref.at[:, columns(1 - core)], own.at[core], twin)
    loads = []
    for at, (src, dst) in enumerate(((gate_ref, gate_buf), (up_ref, up_buf), (down_ref, down_buf))):
        loads.append(pltpu.make_async_copy(src, dst, load_sem.at[at]))
        loads[-1].start()
    kept = ffn_ref[:, columns(core)]
    place = place_ref[...]
    slots = packed.shape[1]
    tail = jnp.dot(place, weight_ref[...], preferred_element_type=jnp.float32)
    for g in range(groups):
        packed[g, :, half:] = tail[g * slots : (g + 1) * slots].astype(jnp.bfloat16)
    swap.wait_recv()
    other = own[1 - core]
    lead = jnp.where(core == 0, kept, other)
    rest = jnp.where(core == 0, other, kept)
    joined = jnp.concatenate([lead, rest], axis=0)
    moved = []
    for cut, body in zip(cuts, thin):
        rows_out = jnp.dot(place, joined[:, body], preferred_element_type=jnp.float32)
        for g in range(groups):
            packed[g, :, body] = rows_out[g * slots : (g + 1) * slots].astype(jnp.bfloat16)
        step = []
        for hop in range(1, groups):
            target = (group + hop) % groups
            step.append(
                send(packed.at[target, :, cut], landed.at[group, :, cut], (target * TOP + member, mine))
            )
        moved.append(step)
        landed[group, :, cut] = packed[group, :, cut]
    beside_x, beside_y, far, shared = [], [], [], []
    for cut, step in zip(cuts, moved):
        for copy in step:
            copy.wait_recv()
        whole = jnp.concatenate(
            [landed[g, :, cut].astype(jnp.float32) for g in range(groups)], axis=0
        )
        slabs[core, member, across, :, cut] = whole.astype(jnp.bfloat16)
        here = slabs.at[core, member, across, :, cut]
        beside_x.append(send(here, here, x_side))
        beside_y.append(send(here, here, y_side))
        shared.append(send(here, here, twin))
    for at, cut in enumerate(cuts):
        from_y = slabs.at[core, member, 1 - across, :, cut]
        from_x = slabs.at[core, 1 - member, across, :, cut]
        beside_y[at].wait_recv()
        if at == 0:
            far.append(send(from_y, from_y, x_side))
        shared.append(send(from_y, from_y, twin))
        beside_x[at].wait_recv()
        if at == 1:
            far.append(send(from_x, from_x, y_side))
    for at, cut in enumerate(cuts):
        from_x = slabs.at[core, 1 - member, across, :, cut]
        shared.append(send(from_x, from_x, twin))
    for copy in loads:
        copy.wait()

    def run(which):
        lefts = [slabs[side, which].reshape(-1, wide) for side in range(2)]
        gate, up = (
            sum(
                jnp.dot(
                    lefts[side][:, :half], buf[side * half : (side + 1) * half],
                    preferred_element_type=jnp.float32,
                )
                for side in range(2)
            )
            for buf in (gate_buf, up_buf)
        )
        hidden = (gate / (1.0 + jnp.exp(-gate)) * up).astype(jnp.bfloat16)
        shares = lefts[0][:, half : half + HEAD].astype(jnp.float32)
        share = jnp.where(
            member == 0, shares[:, 0:1] + shares[:, 1:2], shares[:, 2:3] + shares[:, 3:4]
        )
        for side in range(2):
            for body in thin:
                at = slice(side * half + body.start, side * half + body.stop)
                result = jnp.dot(hidden, down_buf[:, at], preferred_element_type=jnp.float32)
                result = (result * share).astype(jnp.bfloat16)
                outs[side, which, :, :, body] = result.reshape(2, -1, half // 2)

    for copy in shared[:4]:
        copy.wait_recv()
    run(member)
    for at, cut in enumerate(cuts):
        far[at].wait_recv()
        diagonal = slabs.at[core, 1 - member, 1 - across, :, cut]
        shared.append(send(diagonal, diagonal, twin))
    sums = []
    sums.append([
        send(outs.at[1 - core, member, :, :, body], first.at[member, :, :, body], twin)
        for body in thin
    ])
    for copy in shared[4:]:
        copy.wait_recv()
    run(1 - member)
    sums.append([
        send(outs.at[1 - core, 1 - member, :, :, body], first.at[1 - member, :, :, body], twin)
        for body in thin
    ])
    real = jnp.float32
    for copies, which in zip(sums, (member, 1 - member)):
        for copy, body in zip(copies, thin):
            copy.wait_recv()
            added = outs[core, which, :, :, body].astype(real) + first[which, :, :, body].astype(real)
            total[which, :, :, body] = added.astype(jnp.bfloat16)
    diagonal = total.at[1 - member, 1 - across]
    to_y = send(diagonal.at[:, thin[0]], corner.at[0], y_side)
    to_x = send(diagonal.at[:, thin[1]], corner.at[1], x_side)
    x_slab = total.at[1 - member, across]
    y_slab = total.at[member, 1 - across]
    got = [[None, None], [None, None]]
    got[0][1] = send(x_slab.at[:, thin[1]], direct.at[0, :, thin[1]], x_side)
    got[1][0] = send(y_slab.at[:, thin[0]], direct.at[1, :, thin[0]], y_side)
    to_y.wait_recv()
    giving[0] = (total[1 - member, across, :, thin[0]].astype(real) + corner[0].astype(real)).astype(jnp.bfloat16)
    got[0][0] = send(giving.at[0], direct.at[0, :, thin[0]], x_side)
    to_x.wait_recv()
    giving[1] = (total[member, 1 - across, :, thin[1]].astype(real) + corner[1].astype(real)).astype(jnp.bfloat16)
    got[1][1] = send(giving.at[1], direct.at[1, :, thin[1]], y_side)
    returns = []
    for at, body in enumerate(thin):
        got[0][at].wait_recv()
        got[1][at].wait_recv()
        final = (
            total[member, across, :, body].astype(real)
            + direct[0, :, body].astype(real)
            + direct[1, :, body].astype(real)
        )
        for g in range(groups):
            leaving[g, :, body] = final[g * slots : (g + 1) * slots].astype(jnp.bfloat16)
        step = []
        for hop in range(1, groups):
            target = (group + hop) % groups
            step.append(
                send(leaving.at[target, :, body], given.at[group, :, body], (target * TOP + member, mine))
            )
        returns.append(step)
        given[group, :, body] = leaving[group, :, body]
    for body, step in zip(thin, returns):
        for copy in step:
            copy.wait_recv()
        whole = jnp.concatenate([given[g, :, body].astype(real) for g in range(groups)], axis=0)
        back = jnp.dot(back_ref[...], whole.astype(jnp.bfloat16), preferred_element_type=real)
        staged[:, :, body] = back.astype(jnp.bfloat16).reshape(2, rows, half // 2)
    last = send(staged.at[1 - core], blend.at[core], twin)
    squares = jnp.sum(staged[core].astype(real) ** 2, axis=1, keepdims=True)
    last.wait_recv()
    squares += jnp.sum(blend[1 - core].astype(real) ** 2, axis=1, keepdims=True)
    scale = lax.rsqrt(squares / (2 * half) + epsilon)
    for side, source in ((core, staged), (1 - core, blend)):
        at = columns(side)
        out_ref[:, at] = (
            stream_ref[:, at].astype(real) + source[side].astype(real) * scale * gain_ref[:, at]
        ).astype(jnp.bfloat16)
    for copy in sent:
        copy.wait_send()


def layer_part(
    n_sp, n_tp, attended, q_hbm, k_hbm, v_hbm, bias_ref, w_ref, res_hbm, gain_hbm,
    place_ref, back_ref, weight_ref, out_gain_ref, gate_ref, up_ref, down_ref, out_ref,
    stream_ref, ffn_ref, *scratch,
):
    attention_part(
        n_sp, n_tp, q_hbm, k_hbm, v_hbm, bias_ref, w_ref, res_hbm, gain_hbm,
        stream_ref, ffn_ref, *scratch[:attended],
    )
    expert_part(
        place_ref, back_ref, weight_ref, ffn_ref, stream_ref, out_gain_ref,
        gate_ref, up_ref, down_ref, out_ref, *scratch[attended:],
    )


def whole_layer(
    capacity, queries, keys, values, break_bias, w_out, residual, ffn_gain,
    pick_ids, pair_logit, w_gate, w_up, w_down, out_gain,
):
    n_sp, n_tp = lax.axis_size("sp"), lax.axis_size("tp")
    rows, width = residual.shape
    attention = attention_scratch(
        n_sp, n_tp, queries.shape[0], keys.shape[1], queries.shape[1], w_out.shape[1]
    )
    groups = lax.axis_size("sp") // TOP
    across = lax.axis_index("tp") // 2
    chip_rows, slots, half = 2 * rows, 2 * capacity, width // 2
    picks = lax.dynamic_slice_in_dim(pick_ids, across * chip_rows, chip_rows, 0)
    logits = lax.dynamic_slice_in_dim(pair_logit, across * chip_rows, chip_rows, 0)
    chosen = picks[:, 0] // TOP
    at = jnp.arange(chip_rows, dtype=jnp.int32)
    same = (chosen[None, :] == chosen[:, None]) & (at[None, :] < at[:, None])
    target = chosen * slots + jnp.sum(same.astype(jnp.int32), axis=1)
    place = (target[None, :] == jnp.arange(groups * slots, dtype=jnp.int32)[:, None]).astype(jnp.bfloat16)
    sign = jnp.where(picks[:, 0] % TOP == 0, 1.0, -1.0)
    shares = jnp.stack([jax.nn.sigmoid(sign * logits), jax.nn.sigmoid(-sign * logits)], axis=1)
    coarse = lax.reduce_precision(shares, 8, 7)
    parts = jnp.stack([coarse, shares - coarse], axis=2).reshape(chip_rows, 2 * TOP)
    parts = jnp.pad(parts.astype(jnp.bfloat16), ((0, 0), (0, HEAD - 2 * TOP)))
    vmem = pl.BlockSpec(memory_space=pltpu.VMEM)
    hbm = pl.BlockSpec(memory_space=pl.ANY)
    block = groups * slots

    def room(*shape):
        return pltpu.VMEM(shape, jnp.bfloat16)

    dma = pltpu.SemaphoreType.DMA
    return pl.pallas_call(
        functools.partial(layer_part, n_sp, n_tp, len(attention)),
        out_shape=jax.ShapeDtypeStruct(residual.shape, jnp.bfloat16),
        in_specs=[hbm] * 3
        + [pl.BlockSpec(memory_space=pltpu.SMEM)]
        + [hbm] * 3
        + [vmem] * 4
        + [hbm] * 3,
        out_specs=vmem,
        scratch_shapes=[
            room(rows, width), room(rows, width), *attention,
            room(*w_gate.shape), room(*w_up.shape), room(*w_down.shape),
            room(2, rows, half),
            room(groups, slots, half + HEAD),
            room(groups, slots, half + HEAD),
            room(2, TOP, 2, block, half + HEAD),
            room(2, TOP, 2, block, half),
            room(TOP, 2, block, half),
            room(TOP, 2, block, half),
            room(2, block, half // 2),
            room(2, block, half),
            room(2, block, half // 2),
            room(groups, slots, half),
            room(groups, slots, half),
            room(2, rows, half),
            room(2, rows, half),
            dma((3,)), dma((64,)), dma((64,)),
        ],
        compiler_params=pltpu.CompilerParams(
            has_side_effects=True, vmem_limit_bytes=63 * 1024 * 1024
        ),
        name="layer",
    )(
        queries, keys, values, break_bias, w_out, residual, ffn_gain[None],
        place, place.T, parts, out_gain[None], w_gate, w_up, w_down,
    )


def on_device(
    queries,
    keys,
    values,
    break_bias,
    residual,
    w_out,
    ffn_gain,
    pick_ids,
    pair_logit,
    w_gate,
    w_up,
    w_down,
    out_gain,
):
    length = queries.shape[0]
    quarters = lax.axis_size("tp")
    quarter = lax.axis_index("tp")
    slice_rows = length // quarters
    width = w_out.shape[1]
    experts = lax.axis_size("sp")
    capacity = max(TOP, (3 * slice_rows + experts - 1) // experts)
    if experts == GROUPS * TOP and quarters == 4:
        return whole_layer(
            capacity, queries, keys, values, break_bias, w_out, residual, ffn_gain,
            pick_ids, pair_logit, w_gate[0], w_up[0], w_down[0], out_gain,
        )
    stream, ffn_in = attend(queries, keys, values, break_bias, w_out, residual, ffn_gain)
    stream_float = stream.astype(jnp.float32)
    routed = lax.dynamic_slice_in_dim(pick_ids, quarter * slice_rows, slice_rows, 0)[None]
    blocks = routed.shape[0]
    entries = ffn_in.reshape(blocks, slice_rows, width)
    flat_ids = routed.reshape(blocks, slice_rows * TOP)
    places = jnp.arange(slice_rows * TOP, dtype=jnp.int32)
    earlier = places[None, :] < places[:, None]
    matches = (flat_ids[:, :, None] == flat_ids[:, None, :]) & earlier[None]
    ranks = jnp.sum(matches.astype(jnp.int32), axis=2)
    targets = (flat_ids * capacity + ranks).reshape(blocks, slice_rows, TOP)
    block_ids = jnp.arange(blocks, dtype=jnp.int32)[:, None]
    outgoing = jnp.zeros((blocks, experts * capacity, width), jnp.bfloat16)
    for pick_index in range(TOP):
        outgoing = outgoing.at[block_ids, targets[:, :, pick_index]].set(entries)
    arrived = lax.all_to_all(outgoing, "sp", split_axis=1, concat_axis=1, tiled=True).reshape(
        -1, width
    )
    piece = lax.all_gather(arrived, "tp", axis=0, tiled=True)
    gated = jax.nn.silu(jnp.dot(piece, w_gate[0], preferred_element_type=jnp.float32))
    hidden = (gated * jnp.dot(piece, w_up[0], preferred_element_type=jnp.float32)).astype(
        jnp.bfloat16
    )
    results = lax.psum_scatter(
        jnp.dot(hidden, w_down[0], preferred_element_type=jnp.float32).astype(jnp.bfloat16),
        "tp",
        scatter_dimension=0,
        tiled=True,
    )
    returned = lax.all_to_all(results, "sp", split_axis=0, concat_axis=0, tiled=True)
    own_targets = targets[0]
    logits = lax.dynamic_slice_in_dim(pair_logit, quarter * slice_rows, slice_rows, 0)
    leading = returned[own_targets[:, 0]].astype(jnp.float32)
    trailing = returned[own_targets[:, 1]].astype(jnp.float32)
    blended = (
        jax.nn.sigmoid(logits)[:, None] * leading + jax.nn.sigmoid(-logits)[:, None] * trailing
    )
    blend_scale = lax.rsqrt(jnp.mean(blended * blended, axis=-1, keepdims=True) + epsilon)
    return (stream_float + blended * blend_scale * out_gain).astype(jnp.bfloat16)


def solution(mesh):
    placed = (
        P("sp", "tp"),
        P("sp", "tp"),
        P("sp", "tp"),
        P("tp"),
        P(("sp", "tp"), None),
        P("tp", None),
        P(),
        P("sp", None),
        P("sp"),
        P("sp", None, "tp"),
        P("sp", None, "tp"),
        P("sp", "tp", None),
        P(),
    )
    return jax.shard_map(
        on_device, mesh=mesh, in_specs=placed, out_specs=P(("sp", "tp"), None), check_vma=False
    )
```
